512 devices in a mesh: sp: 32 (over z, x), tp: 16 (over y, core).
Axes of the slice: x: 4, y: 8, z: 8, core: 2. Of those that a mesh axis runs over, the one named last changes fastest.
Arguments:
- tokens: bfloat16 [32, 3072, 2048], P('sp', 'tp'), may hold values from -100 to 100
- norm_gain: float32 [2048], replicated, may hold values from 0.1 to 1.9
- key_weight: bfloat16 [2048, 1024], P('sp', 'tp'), may hold values from -0.125 to 0.125
- value_weight: bfloat16 [2048, 1024], P('sp', 'tp'), may hold values from -0.125 to 0.125
- cum_gate: float32 [32, 32, 3072], P('sp', None, 'tp'), may hold values from -448 to 0, as said below
- new_gate: float32 [32, 32], P('sp', 'tp'), may hold values from -448 to 0
- new_query: bfloat16 [32, 2048], P('sp', 'tp'), may hold values from -128 to 128
- new_kv: bfloat16 [32, 16, 128], P('sp', 'tp'), may hold values from -4 to 4
Outputs:
- kv_cache: bfloat16 [32, 16, 3072, 128], P('sp', 'tp')
- gate_log_cache: float32 [32, 32, 3072], P('sp', 'tp')
- read_out: bfloat16 [32, 2048], P('sp', 'tp')
The draws below stay inside these ranges and needn't reach their ends.
Inputs may be any that keep to these rules, and one draw needn't show every extreme that they name: Along positions cum_gate never rises; new_gate is at most the last position's value of its prompt and head.
All inputs are finite; a program needn't handle non-finite values.
Results may differ from the reference program's by a relative error of at most 0.0071.
Values may be sent and summed in bfloat16 or wider, within the bound.
No kernel may reach another device: no remote copies, remote signals or barrier semaphores. Data moves between devices by JAX's collectives and lax.ppermute only.
A program may use at most 64 MiB of HBM per device.

```python
import math
import jax
import jax.numpy as jnp
from jax import lax

D = 2048
HEADS = 32
KV_HEADS = 16
HEAD = 64
POS_DEV = 192
SEQS = 32
PROMPT_LENGTH = 3072


def gate_table(key):
    key_slow = jax.random.fold_in(key, 101)
    key_rate = jax.random.fold_in(key, 102)
    key_block = jax.random.fold_in(key, 103)
    key_place = jax.random.fold_in(key, 104)
    key_random_split = jax.random.fold_in(key, 105)
    key_layer_count = jax.random.fold_in(key, 106)
    slow_share = 0.5
    slow = jax.random.uniform(key_slow, (SEQS, HEADS, 1), jnp.float32) < slow_share
    scatter_update = jnp.exp(jax.random.uniform(key_rate, (SEQS, HEADS, 1), jnp.float32, jnp.log(0.5), jnp.log(2.0)))
    base = jnp.where(slow, scatter_update / PROMPT_LENGTH, scatter_update * 0.8 / 40.0)
    blocks = PROMPT_LENGTH // POS_DEV + 1
    block_table = jnp.exp(jax.random.uniform(key_block, (SEQS, 1, blocks), jnp.float32, jnp.log(0.5), jnp.log(2.0)))
    block_rate = jnp.repeat(block_table, POS_DEV, axis=2)[:, :, :PROMPT_LENGTH + 1]
    place = jax.random.uniform(key_place, (SEQS, HEADS, PROMPT_LENGTH + 1), jnp.float32, 0.3, 1.7)
    logs = -base * block_rate * place
    slot_locations = jax.random.randint(key_random_split, (4,), 0, PROMPT_LENGTH)
    hit = jnp.any(jnp.arange(PROMPT_LENGTH + 1)[:, None] == slot_locations[None, :], axis=1)
    depth = jnp.log(jax.random.uniform(key_layer_count, (SEQS, HEADS, 1), jnp.float32, 0.5, 0.8))
    logs = logs + jnp.where(hit[None, None, :] & slow, depth, 0.0)
    return jnp.cumsum(logs, axis=2)


def draw_cum_gate(key, part):
    return gate_table(key)[:, :, :PROMPT_LENGTH]


def draw_new_gate(key, part):
    return gate_table(key)[:, :, PROMPT_LENGTH]


def draw_tokens(key, part):
    key_main = jax.random.fold_in(key, 201)
    column_scale = 0.5 * 4.0 ** (jnp.arange(D, dtype=jnp.float32) / D)
    values = jax.random.truncated_normal(key_main, -4.0, 4.0, (SEQS, PROMPT_LENGTH, D), jnp.float32) * column_scale
    return values.astype(jnp.bfloat16)


def updated_page_table(key):
    key_kv = jax.random.fold_in(key, 301)
    key_query = jax.random.fold_in(key, 302)
    fresh_kv = jax.random.truncated_normal(key_kv, -4.0, 4.0, (SEQS, KV_HEADS, 2 * HEAD), jnp.float32)
    query = jax.random.truncated_normal(key_query, -4.0, 4.0, (SEQS, HEADS, HEAD), jnp.float32)
    return (query.reshape(SEQS, HEADS * HEAD), fresh_kv)


def draw_new_query(key, part):
    return updated_page_table(jax.random.fold_in(key, 300))[0].astype(jnp.bfloat16)


def draw_new_kv(key, part):
    return updated_page_table(jax.random.fold_in(key, 300))[1].astype(jnp.bfloat16)


def level_of(key, dims, shards, low, high):
    def one(dim, shards_of):
        steps = jax.random.uniform(jax.random.fold_in(jax.random.fold_in(key, 6), dim), (shards_of,), jnp.float32, low / len(shards), high / len(shards))
        return jnp.repeat(jnp.exp(steps), dims[dim] // shards_of).reshape((-1,) + (1,) * (len(dims) - dim - 1))

    gain = one(*shards[0])
    for cut in shards[1:]:
        gain = gain * one(*cut)
    return gain


def normal_values(key, dims, deviation, bound, split=(), held_as=jnp.bfloat16):
    factor_of = level_of(key, dims, split, -0.22, 0.18) if split else 1.0
    values = jax.random.normal(key, dims, jnp.float32) * deviation * factor_of
    return jnp.minimum(jnp.maximum(values, -bound), bound).astype(held_as)


def setup_inputs(seed: int = 0) -> dict:
    key_of = jax.random.split(jax.random.key(seed), 9)
    return {
        "tokens": draw_tokens(jax.random.fold_in(key_of[8], 71), 0),
        "norm_gain": jnp.clip(1.0 + 0.18 * jax.random.normal(key_of[1], (D,), jnp.float32), 0.1, 1.9),
        "key_weight": normal_values(key_of[2], (D, KV_HEADS * HEAD), D ** -0.5, 0.125, ((0, 32), (1, 16))),
        "value_weight": normal_values(key_of[3], (D, KV_HEADS * HEAD), D ** -0.5, 0.125, ((0, 32), (1, 16))),
        "cum_gate": draw_cum_gate(jax.random.fold_in(key_of[8], 71), 0),
        "new_gate": draw_new_gate(jax.random.fold_in(key_of[8], 71), 0),
        "new_query": draw_new_query(jax.random.fold_in(key_of[8], 71), 0),
        "new_kv": draw_new_kv(jax.random.fold_in(key_of[8], 71), 0),
    }


def reference(tokens, norm_gain, key_weight, value_weight, cum_gate, new_gate, new_query, new_kv):
    scale_factor = 1.0 / math.sqrt(HEAD)
    group = HEADS // KV_HEADS

    def one_prompt(inputs):
        rows, gate_rows, fresh_gate, fresh_query, fresh_kv = inputs
        length = rows.shape[0]
        widened = rows.astype(jnp.float32)
        inv_rms = lax.rsqrt(lax.optimization_barrier(jnp.mean(widened * widened, axis=1, keepdims=True)) + 1e-06)
        scaled = (widened * norm_gain).astype(jnp.bfloat16)
        keys = (jnp.dot(scaled, key_weight, preferred_element_type=jnp.float32) * inv_rms).astype(jnp.bfloat16)
        values = (jnp.dot(scaled, value_weight, preferred_element_type=jnp.float32) * inv_rms).astype(jnp.bfloat16)
        key_heads = keys.reshape(length, KV_HEADS, HEAD)
        value_heads = values.reshape(length, KV_HEADS, HEAD)
        cache = jnp.transpose(jnp.concatenate([key_heads, value_heads], axis=2), (1, 0, 2))
        query = fresh_query.astype(jnp.float32).reshape(KV_HEADS, group, HEAD)
        own_key = fresh_kv[:, :HEAD].astype(jnp.float32)
        own_value = fresh_kv[:, HEAD:].astype(jnp.float32)
        score = jnp.einsum('tkd,kgd->kgt', key_heads.astype(jnp.float32), query) * scale_factor
        score = score + fresh_gate.reshape(KV_HEADS, group)[:, :, None] - gate_rows.reshape(KV_HEADS, group, length)
        own = lax.optimization_barrier(jnp.sum(query * own_key[:, None, :], axis=2)) * scale_factor
        top = jnp.maximum(lax.optimization_barrier(jnp.max(score, axis=2)), own)
        expo = jnp.exp(score - top[:, :, None])
        own_factor = jnp.exp(own - top)
        total = lax.optimization_barrier(jnp.sum(expo, axis=2)) + own_factor
        weights = lax.optimization_barrier(expo.astype(jnp.bfloat16)).astype(jnp.float32)
        numer = jnp.einsum('kgt,tkd->kgd', weights, value_heads.astype(jnp.float32))
        numer = numer + own_factor[:, :, None] * own_value[:, None, :]
        result = (numer / total[:, :, None]).reshape(HEADS * HEAD).astype(jnp.bfloat16)
        return (cache, result)
    kv_cache, read_out = lax.map(one_prompt, (tokens, cum_gate, new_gate, new_query, new_kv))
    return (kv_cache, cum_gate, read_out)
```

```python
import functools
import math

import jax
import jax.numpy as jnp
from jax import lax
from jax.experimental import pallas as pl
from jax.experimental.pallas import tpu as pltpu
from jax.sharding import Mesh, PartitionSpec as P

HEAD = 64
RING = 8


def ring_pairs(step):
    return [(i, (i + step) % RING) for i in range(RING)]


SWAP = [(0, 1), (1, 0)]


def project_body(count, *refs):
    rows = refs[:count]
    gain, mine, other = refs[count : count + 3]
    out_mine, out_other = refs[count + 3 :]
    height = rows[0].shape[0]
    for k, ref in enumerate(rows):
        wide = ref[...].astype(jnp.float32)
        inv_rms = lax.rsqrt(jnp.mean(wide * wide, axis=1, keepdims=True) + 1e-06)
        scaled = (wide * gain[...]).astype(jnp.bfloat16)
        for weight, out in ((mine, out_mine), (other, out_other)):
            product = jnp.dot(scaled, weight[...], preferred_element_type=jnp.float32)
            out[k * height : (k + 1) * height, :] = (product * inv_rms).astype(jnp.bfloat16)


def project(rows, gain, mine, other):
    height = sum(r.shape[0] for r in rows)
    shape = jax.ShapeDtypeStruct((height, 2 * HEAD), jnp.bfloat16)
    return pl.pallas_call(
        functools.partial(project_body, len(rows)),
        out_shape=(shape, shape),
        cost_estimate=pl.CostEstimate(
            flops=height * 2048 * 512, bytes_accessed=height * 2048 * 2, transcendentals=0
        ),
    )(*rows, gain, mine, other)


def finish_body(place, *refs):
    where = refs[0]
    pieces = refs[1:9]
    gate, fresh_gate, query, fresh = refs[9:13]
    cache, read = refs[13:]
    at, core = where[0], where[1]
    for k, ref in enumerate(pieces):
        side = core if k < 4 else 1 - core
        for row, height, shift, offset in place[k % 4]:
            start = ((at + shift) % RING * 2 + side) * 192 + offset
            start = pl.multiple_of(start, 32)
            cache[pl.ds(start, height), :] = ref[row : row + height, :]
    factor = 1.0 / math.sqrt(HEAD)
    lane = lax.broadcasted_iota(jnp.int32, (2, 2 * HEAD), 1)
    head = lax.broadcasted_iota(jnp.int32, (2, 2 * HEAD), 0)
    both = jnp.broadcast_to(query[...].astype(jnp.float32), (2, 2 * HEAD))
    first = jnp.where(head == 0, both, pltpu.roll(both, HEAD, 1))
    keyed = jnp.where(lane < HEAD, first, 0.0)
    new = jnp.broadcast_to(fresh[...].astype(jnp.float32), (2, 2 * HEAD))
    own = jnp.sum(keyed * new, axis=1, keepdims=True) * factor
    whole = cache[...]
    score = (
        lax.dot_general(
            keyed.astype(jnp.bfloat16),
            whole,
            (((1,), (1,)), ((), ())),
            preferred_element_type=jnp.float32,
        )
        * factor
    )
    score = score + fresh_gate[...] - gate[...]
    top = jnp.maximum(jnp.max(score, axis=1, keepdims=True), own)
    expo = jnp.exp(score - top)
    own_factor = jnp.exp(own - top)
    total = jnp.sum(expo, axis=1, keepdims=True) + own_factor
    numer = jnp.dot(expo.astype(jnp.bfloat16), whole, preferred_element_type=jnp.float32)
    result = (numer + own_factor * new) / total
    moved = pltpu.roll(result, HEAD, 1)
    read[...] = jnp.where(lane[:1] < HEAD, moved[:1], result[1:]).astype(jnp.bfloat16)


def finish(place, where, pieces, gate, fresh_gate, query, fresh):
    smem = pl.BlockSpec(memory_space=pltpu.SMEM)
    vmem = pl.BlockSpec(memory_space=pltpu.VMEM)
    return pl.pallas_call(
        functools.partial(finish_body, place),
        out_shape=(
            jax.ShapeDtypeStruct((3072, 2 * HEAD), jnp.bfloat16),
            jax.ShapeDtypeStruct((1, 2 * HEAD), jnp.bfloat16),
        ),
        in_specs=[smem] + [vmem] * 12,
        out_specs=(vmem, vmem),
    )(where, *pieces, gate, fresh_gate, query, fresh)


def per_device(tokens, norm_gain, key_weight, value_weight, cum_gate, new_gate, new_query, new_kv):
    block = tokens[0]
    half = block.shape[0] // 2
    up, down = ring_pairs(1), ring_pairs(-1)
    halves = (block[:half], block[half:])
    fwd = {0: list(halves)}
    bwd = {0: list(halves)}
    for step in (1, 2, 3):
        fwd[step] = [None, None]
        bwd[step] = [None, None]
        for part in (0, 1):
            fwd[step][part] = lax.ppermute(fwd[step - 1][part], "y", up)
            bwd[step][part] = lax.ppermute(bwd[step - 1][part], "y", down)
    far = [lax.ppermute(fwd[3][0], "y", up), lax.ppermute(bwd[3][1], "y", down)]

    local = jnp.concatenate([key_weight, value_weight], axis=1)
    spread = jnp.broadcast_to(local[None], (32,) + local.shape)
    mine = lax.all_to_all(spread, ("z", "x"), 0, 0, tiled=True).reshape(2048, 2 * HEAD)
    other = lax.ppermute(mine, "c", SWAP)
    gate_here = lax.all_to_all(cum_gate, ("y", "c"), split_axis=1, concat_axis=2, tiled=True)

    gain = norm_gain.reshape(1, -1)
    groups = [list(halves) + fwd[1] + bwd[1], fwd[2] + bwd[2], fwd[3] + bwd[3], far]
    kept, swapped = [], []
    for group in groups:
        a, b = project(group, gain, mine, other)
        kept.append(a)
        swapped.append(lax.ppermute(b, "c", SWAP))
    place = [
        [(0, 192, 0, 0), (192, 192, RING - 1, 0), (384, 192, 1, 0)],
        [(0, 192, RING - 2, 0), (192, 192, 2, 0)],
        [(0, 192, RING - 3, 0), (192, 192, 3, 0)],
        [(0, 192, 4, 0)],
    ]
    where = jnp.stack([lax.axis_index("y"), lax.axis_index("c")]).astype(jnp.int32)
    cache, read = finish(
        place, where, kept + swapped, gate_here[0], new_gate.reshape(2, 1), new_query, new_kv[0]
    )
    return (cache[None, None], gate_here, read)


def solution(mesh):
    fine = Mesh(mesh.devices.reshape(8, 4, 8, 2), ("z", "x", "y", "c"))
    sp, tp = ("z", "x"), ("y", "c")
    in_specs = (
        P(sp, tp, None),
        P(),
        P(sp, tp),
        P(sp, tp),
        P(sp, None, tp),
        P(sp, tp),
        P(sp, tp),
        P(sp, tp, None),
    )
    out_specs = (P(sp, tp, None, None), P(sp, tp, None), P(sp, tp))
    return jax.shard_map(
        per_device, mesh=fine, in_specs=in_specs, out_specs=out_specs, check_vma=False
    )
```

```python
import functools
import math

import jax
import jax.numpy as jnp
from jax import lax
from jax.experimental import pallas as pl
from jax.experimental.pallas import tpu as pltpu
from jax.sharding import Mesh, PartitionSpec as P

HEAD = 64
WIDE = 2 * HEAD
RING = 8
POS = 192
AHEAD = [(2 * y + c, 2 * ((y + 1 - 2 * c) % RING) + c) for y in range(RING) for c in (0, 1)]
SWAP = [(0, 1), (1, 0)]
KINDS = (((0, 0), (1, 0), (1, 1), (2, 0), (2, 1)), ((3, 0), (3, 1)), ((4, 0),))
VMEM = pl.BlockSpec(memory_space=pltpu.VMEM)
LIMIT = pltpu.CompilerParams(vmem_limit_bytes=16 * 2**20)


def on_chip(array):
    return pltpu.with_memory_space_constraint(array, pltpu.VMEM)


def project_body(count, *refs):
    rows = refs[:count]
    gain, mine, other = refs[count : count + 3]
    before = refs[count + 3 : -2]
    out_mine, out_other = refs[-2:]
    held = 0
    for ref in before:
        out_other[held : held + ref.shape[0], :] = ref[...]
        held += ref.shape[0]
    for k, ref in enumerate(rows):
        wide = ref[...].astype(jnp.float32)
        inv_rms = lax.rsqrt(jnp.mean(wide * wide, axis=1, keepdims=True) + 1e-06)
        scaled = (wide * gain[...]).astype(jnp.bfloat16)
        for weight, out, skip in ((mine, out_mine, 0), (other, out_other, held)):
            product = jnp.dot(scaled, weight[...], preferred_element_type=jnp.float32)
            at = skip + k * POS
            out[at : at + POS, :] = (product * inv_rms).astype(jnp.bfloat16)


def project(rows, gain, weights, before=()):
    height = POS * len(rows)
    held = sum(b.shape[0] for b in before)
    return pl.pallas_call(
        functools.partial(project_body, len(rows)),
        out_shape=(
            pltpu.VMEM((height, WIDE), jnp.bfloat16),
            pltpu.VMEM((held + height, WIDE), jnp.bfloat16),
        ),
        in_specs=[VMEM] * (len(rows) + 3 + len(before)),
        out_specs=(VMEM, VMEM),
        compiler_params=LIMIT,
        cost_estimate=pl.CostEstimate(
            flops=height * 2048 * 512, bytes_accessed=height * 2048 * 2, transcendentals=0
        ),
    )(*rows, gain, *weights, *before)


def finish_body(gates, small, *refs):
    pieces = refs[:4]
    cache, gate_out, read, sems = refs[4:]
    at, core = lax.axis_index("y"), lax.axis_index("c")
    way = 1 - 2 * core
    blocks, copies = [], []
    kinds = KINDS + (sum(KINDS, ()),)
    for k, ref in enumerate(pieces):
        partner = k // 3
        sign = way * (2 * partner - 1)
        for row, (hops, crossed) in enumerate(kinds[k]):
            side = (core + partner + crossed) % 2
            place = (at + sign * hops + RING) % RING * 2 + side
            block = ref.at[row * POS : (row + 1) * POS, :]
            start = pl.multiple_of(place * POS, POS)
            copy = pltpu.make_async_copy(block, cache.at[pl.ds(start, POS), :], sems.at[len(copies)])
            copy.start()
            copies.append(copy)
            blocks.append((block, place))
    gate_out[...] = jnp.concatenate([gates[p] for p in range(2 * RING)], axis=1)
    factor = 1.0 / math.sqrt(HEAD)
    lane = lax.broadcasted_iota(jnp.int32, (2, WIDE), 1)
    head = lax.broadcasted_iota(jnp.int32, (2, WIDE), 0)
    both = jnp.broadcast_to(small[0:1, :], (2, WIDE))
    new = jnp.broadcast_to(small[1:2, :], (2, WIDE))
    fresh = jnp.sum(jnp.where(lane == head, small[2:3, :], 0.0), axis=1, keepdims=True)
    keyed = jnp.where(lane < HEAD, jnp.where(head == 0, both, pltpu.roll(both, HEAD, 1)), 0.0)
    own = jnp.sum(keyed * new, axis=1, keepdims=True) * factor
    query = keyed.astype(jnp.bfloat16)
    scores = []
    for block, place in blocks:
        raw = lax.dot_general(
            query, block[...], (((1,), (1,)), ((), ())), preferred_element_type=jnp.float32
        )
        scores.append(raw * factor + fresh - gates[place])
    peak = functools.reduce(jnp.maximum, scores)
    top = jnp.maximum(jnp.max(peak, axis=1, keepdims=True), own)
    own_factor = jnp.exp(own - top)
    total = jnp.zeros((2, POS), jnp.float32)
    numer = own_factor * new
    for (block, _), score in zip(blocks, scores):
        expo = jnp.exp(score - top)
        total += expo
        numer += jnp.dot(expo.astype(jnp.bfloat16), block[...], preferred_element_type=jnp.float32)
    result = numer / (jnp.sum(total, axis=1, keepdims=True) + own_factor)
    shifted = pltpu.roll(result, HEAD, 1)
    read[...] = jnp.where(lane[:1] < HEAD, shifted[:1], result[1:]).astype(jnp.bfloat16)
    for copy in copies:
        copy.wait()


def finish(gates, small, pieces):
    return pl.pallas_call(
        finish_body,
        out_shape=(
            jax.ShapeDtypeStruct((2 * RING * POS, WIDE), jnp.bfloat16),
            jax.ShapeDtypeStruct((2, 2 * RING * POS), jnp.float32),
            jax.ShapeDtypeStruct((1, WIDE), jnp.bfloat16),
        ),
        in_specs=[VMEM] * 6,
        out_specs=(pl.BlockSpec(memory_space=pl.ANY), VMEM, VMEM),
        scratch_shapes=[pltpu.SemaphoreType.DMA((2 * RING,))],
        compiler_params=LIMIT,
    )(on_chip(gates), on_chip(small), *[on_chip(p) for p in pieces])


def per_device(tokens, norm_gain, key_weight, value_weight, cum_gate, new_gate, new_query, new_kv):
    block = tokens[0]
    tp = ("y", "c")
    ahead = [lax.ppermute(block, tp, AHEAD)]

    local = jnp.concatenate([key_weight, value_weight], axis=1)
    spread = jnp.broadcast_to(local[None], (32,) + local.shape)
    gain = jnp.broadcast_to(norm_gain[None], (1, 2048))
    small = jnp.concatenate(
        [
            new_query.astype(jnp.float32),
            new_kv[0].astype(jnp.float32),
            jnp.pad(new_gate, ((0, 0), (0, WIDE - 2))),
        ],
        axis=0,
    )
    gate_parts = cum_gate[0].reshape(2 * RING, 2, POS)
    fellow = lax.ppermute(block, "c", SWAP)
    fellow, gain, small, gate_parts, spread = lax.optimization_barrier(
        (fellow, gain, small, gate_parts, spread)
    )
    crossed = [lax.ppermute(fellow, tp, AHEAD)]
    gathered = lax.all_to_all(spread, ("z", "x"), 0, 0, tiled=True)
    mine = gathered.reshape(2048, WIDE)
    weights = [on_chip(mine), on_chip(lax.ppermute(mine, "c", SWAP))]

    for step in (2, 3, 4):
        ahead.append(lax.ppermute(ahead[-1], tp, AHEAD))
        if step < 4:
            crossed.append(lax.ppermute(crossed[-1], tp, AHEAD))
    gates = lax.all_to_all(gate_parts, tp, split_axis=0, concat_axis=0, tiled=True)

    gain = on_chip(gain)
    first = [block] + [on_chip(r) for r in (ahead[0], crossed[0], ahead[1], crossed[1])]
    kept0, other0 = project(first, gain, weights)
    kept1, other1 = project([on_chip(ahead[2]), on_chip(crossed[2])], gain, weights)
    before = [on_chip(other0), on_chip(other1)]
    kept2, others = project([on_chip(ahead[3])], gain, weights, before)
    swapped = lax.ppermute(others, "c", SWAP)
    cache, gate_out, read = finish(gates, small, (kept0, kept1, kept2, swapped))
    return (cache[None, None], gate_out[None], read)


def solution(mesh):
    fine = Mesh(mesh.devices.reshape(8, 4, 8, 2), ("z", "x", "y", "c"))
    sp, tp = ("z", "x"), ("y", "c")
    in_specs = (
        P(sp, tp, None),
        P(),
        P(sp, tp),
        P(sp, tp),
        P(sp, None, tp),
        P(sp, tp),
        P(sp, tp),
        P(sp, tp, None),
    )
    out_specs = (P(sp, tp, None, None), P(sp, tp, None), P(sp, tp))
    return jax.shard_map(
        per_device, mesh=fine, in_specs=in_specs, out_specs=out_specs, check_vma=False
    )
```

```python
import functools
import math

import jax
import jax.numpy as jnp
from jax import lax
from jax.experimental import pallas as pl
from jax.experimental.pallas import tpu as pltpu
from jax.sharding import Mesh, PartitionSpec as P

HEAD = 64
WIDE = 2 * HEAD
RING = 8
POS = 192
AHEAD = [(2 * y + c, 2 * ((y + 1 - 2 * c) % RING) + c) for y in range(RING) for c in (0, 1)]
SWAP = [(0, 1), (1, 0)]
FACTOR = 1.0 / math.sqrt(HEAD)
EARLY = ((0, 0), (1, 0), (1, 1), (2, 0), (2, 1), (3, 0), (3, 1))
LATE = ((4, 0),)
VMEM = pl.BlockSpec(memory_space=pltpu.VMEM)
ANY = pl.BlockSpec(memory_space=pl.ANY)
LIMIT = pltpu.CompilerParams(vmem_limit_bytes=16 * 2**20)


def on_chip(array):
    return pltpu.with_memory_space_constraint(array, pltpu.VMEM)


def project_block(rows, gain, mine, other, out_mine, out_other, at_mine, at_other):
    height = rows.shape[0]
    wide = rows.astype(jnp.float32)
    inv_rms = lax.rsqrt(jnp.mean(wide * wide, axis=1, keepdims=True) + 1e-06)
    scaled = (wide * gain[...]).astype(jnp.bfloat16)
    for weight, out, at in ((mine, out_mine, at_mine), (other, out_other, at_other)):
        product = jnp.dot(scaled, weight[...], preferred_element_type=jnp.float32)
        out[at : at + height, :] = (product * inv_rms).astype(jnp.bfloat16)


def early_body(count, *refs):
    rows = refs[:count]
    gain, mine, other, cache, out_mine, out_other, held, sems, out_sems = refs[count:]
    copies = [pltpu.make_async_copy(r, held.at[k], sems.at[k]) for k, r in enumerate(rows)]
    for copy in copies:
        copy.start()
    where = places(EARLY, 0)
    stores = []
    for k, copy in enumerate(copies):
        copy.wait()
        project_block(held[k], gain, mine, other, out_mine, out_other, k * POS, k * POS)
        stores.append(store_block(out_mine, k, where[k], cache, out_sems.at[k]))
    for store in stores:
        store.wait()


def project_early(rows, gain, weights):
    count = len(rows)
    height = POS * count
    shape = pltpu.VMEM((height, WIDE), jnp.bfloat16)
    return pl.pallas_call(
        functools.partial(early_body, count),
        out_shape=(jax.ShapeDtypeStruct((2 * RING * POS, WIDE), jnp.bfloat16), shape, shape),
        in_specs=[ANY] * count + [VMEM] * 3,
        out_specs=(ANY, VMEM, VMEM),
        scratch_shapes=[
            pltpu.VMEM((count, POS, 2048), jnp.bfloat16),
            pltpu.SemaphoreType.DMA((count,)),
            pltpu.SemaphoreType.DMA((count,)),
        ],
        compiler_params=LIMIT,
        cost_estimate=pl.CostEstimate(
            flops=height * 2048 * 512, bytes_accessed=height * 2048 * 2, transcendentals=0
        ),
    )(*rows, gain, *weights)


def late_body(rows, gain, mine, other, before, out_mine, out_other):
    held = before.shape[0]
    out_other[:held, :] = before[...]
    project_block(rows[...], gain, mine, other, out_mine, out_other, 0, held)


def project_late(rows, gain, weights, before):
    return pl.pallas_call(
        late_body,
        out_shape=(
            pltpu.VMEM((POS, WIDE), jnp.bfloat16),
            pltpu.VMEM((before.shape[0] + POS, WIDE), jnp.bfloat16),
        ),
        in_specs=[VMEM] * 5,
        out_specs=(VMEM, VMEM),
        compiler_params=LIMIT,
    )(rows, gain, *weights, before)


def places(kinds, partner):
    at, core = lax.axis_index("y"), lax.axis_index("c")
    sign = (1 - 2 * core) * (2 * partner - 1)
    return [
        (at + sign * hops + RING) % RING * 2 + (core + partner + crossed) % 2
        for hops, crossed in kinds
    ]


def store_block(ref, row, place, cache, sem):
    block = ref.at[row * POS : (row + 1) * POS, :]
    start = pl.multiple_of(place * POS, POS)
    copy = pltpu.make_async_copy(block, cache.at[pl.ds(start, POS), :], sem)
    copy.start()
    return copy


def read_parts(small):
    lane = lax.broadcasted_iota(jnp.int32, (2, WIDE), 1)
    head = lax.broadcasted_iota(jnp.int32, (2, WIDE), 0)
    both = jnp.broadcast_to(small[0:1, :], (2, WIDE))
    new = jnp.broadcast_to(small[1:2, :], (2, WIDE))
    fresh = jnp.sum(jnp.where(lane == head, small[2:3, :], 0.0), axis=1, keepdims=True)
    keyed = jnp.where(lane < HEAD, jnp.where(head == 0, both, pltpu.roll(both, HEAD, 1)), 0.0)
    own = jnp.sum(keyed * new, axis=1, keepdims=True) * FACTOR
    return keyed.astype(jnp.bfloat16), new, own, fresh


def finish_body(gates, small, early, late, swapped, cache_in, cache, gate_out, read, sems):
    del cache_in
    heres, here, there = places(EARLY, 0), places(LATE, 0), places(EARLY + LATE, 1)
    copies = []
    for ref, where in ((late, here), (swapped, there)):
        for row, place in enumerate(where):
            copies.append(store_block(ref, row, place, cache, sems.at[len(copies)]))
    gate_out[...] = jnp.concatenate([gates[p] for p in range(2 * RING)], axis=1)
    query, new, own, fresh = read_parts(small)
    top, scores = own, []
    for ref, where in ((early, heres), (late, here), (swapped, there)):
        raw = lax.dot_general(
            query, ref[...], (((1,), (1,)), ((), ())), preferred_element_type=jnp.float32
        )
        gate = jnp.concatenate([gates[place] for place in where], axis=1)
        scores.append(raw * FACTOR + fresh - gate)
        top = jnp.maximum(top, jnp.max(scores[-1], axis=1, keepdims=True))
    total = jnp.exp(own - top)
    numer = total * new
    for ref, score in zip((early, late, swapped), scores):
        expo = jnp.exp(score - top)
        total += jnp.sum(expo, axis=1, keepdims=True)
        numer += jnp.dot(
            expo.astype(jnp.bfloat16), ref[...], preferred_element_type=jnp.float32
        )
    result = numer / total
    lane = lax.broadcasted_iota(jnp.int32, (1, WIDE), 1)
    shifted = pltpu.roll(result, HEAD, 1)
    read[...] = jnp.where(lane < HEAD, shifted[:1], result[1:]).astype(jnp.bfloat16)
    for copy in copies:
        copy.wait()


def finish(gates, small, early, late, swapped, cache):
    return pl.pallas_call(
        finish_body,
        out_shape=(
            jax.ShapeDtypeStruct((2 * RING * POS, WIDE), jnp.bfloat16),
            jax.ShapeDtypeStruct((2, 2 * RING * POS), jnp.float32),
            jax.ShapeDtypeStruct((1, WIDE), jnp.bfloat16),
        ),
        in_specs=[VMEM] * 5 + [ANY],
        out_specs=(ANY, VMEM, VMEM),
        scratch_shapes=[pltpu.SemaphoreType.DMA((len(EARLY) + 2 * len(LATE),))],
        input_output_aliases={5: 0},
        compiler_params=LIMIT,
    )(on_chip(gates), on_chip(small), on_chip(early), on_chip(late), on_chip(swapped), cache)


def per_device(tokens, norm_gain, key_weight, value_weight, cum_gate, new_gate, new_query, new_kv):
    block = tokens[0]
    tp = ("y", "c")
    ahead = [lax.ppermute(block, tp, AHEAD)]

    local = jnp.concatenate([key_weight, value_weight], axis=1)
    spread = jnp.broadcast_to(local[None], (32,) + local.shape)
    gain = jnp.broadcast_to(norm_gain[None], (1, 2048))
    small = jnp.concatenate(
        [
            new_query.astype(jnp.float32),
            new_kv[0].astype(jnp.float32),
            jnp.pad(new_gate, ((0, 0), (0, WIDE - 2))),
        ],
        axis=0,
    )
    gate_parts = cum_gate[0].reshape(2 * RING, 2, POS)
    fellow = lax.ppermute(block, "c", SWAP)
    fellow, gain, small, gate_parts, spread = lax.optimization_barrier(
        (fellow, gain, small, gate_parts, spread)
    )
    crossed = [lax.ppermute(fellow, tp, AHEAD)]
    gathered = lax.all_to_all(spread, ("z", "x"), 0, 0, tiled=True)
    mine = gathered.reshape(2048, WIDE)
    weights = [on_chip(mine), on_chip(lax.ppermute(mine, "c", SWAP))]

    for step in (2, 3, 4):
        ahead.append(lax.ppermute(ahead[-1], tp, AHEAD))
        if step < 4:
            crossed.append(lax.ppermute(crossed[-1], tp, AHEAD))
    gates = lax.all_to_all(gate_parts, tp, split_axis=0, concat_axis=0, tiled=True)

    gain = on_chip(gain)
    first = [block]
    for pair in zip(ahead, crossed):
        first += pair
    cache, early, other = project_early(first, gain, weights)
    late, others = project_late(on_chip(ahead[3]), gain, weights, on_chip(other))
    swapped = lax.ppermute(others, "c", SWAP)
    cache, gate_out, read = finish(gates, small, early, late, swapped, cache)
    return (cache[None, None], gate_out[None], read)


def solution(mesh):
    fine = Mesh(mesh.devices.reshape(8, 4, 8, 2), ("z", "x", "y", "c"))
    sp, tp = ("z", "x"), ("y", "c")
    in_specs = (
        P(sp, tp, None),
        P(),
        P(sp, tp),
        P(sp, tp),
        P(sp, None, tp),
        P(sp, tp),
        P(sp, tp),
        P(sp, tp, None),
    )
    out_specs = (P(sp, tp, None, None), P(sp, tp, None), P(sp, tp))
    return jax.shard_map(
        per_device, mesh=fine, in_specs=in_specs, out_specs=out_specs, check_vma=False
    )
```

```python
import functools
import math

import jax
import jax.numpy as jnp
from jax import lax
from jax.experimental import pallas as pl
from jax.experimental.pallas import tpu as pltpu
from jax.sharding import Mesh, PartitionSpec as P

HEAD = 64
WIDE = 2 * HEAD
RING = 8
POS = 192
AHEAD = [(2 * y + c, 2 * ((y + 1 - 2 * c) % RING) + c) for y in range(RING) for c in (0, 1)]
SWAP = [(0, 1), (1, 0)]
FACTOR = 1.0 / math.sqrt(HEAD)
EARLY = ((0, 0), (1, 0), (1, 1), (2, 0), (2, 1), (3, 0), (3, 1))
LATE = ((4, 0),)
VMEM = pl.BlockSpec(memory_space=pltpu.VMEM)
ANY = pl.BlockSpec(memory_space=pl.ANY)
LIMIT = pltpu.CompilerParams(vmem_limit_bytes=16 * 2**20)


def on_chip(array):
    return pltpu.with_memory_space_constraint(array, pltpu.VMEM)


def project_block(rows, gain, mine, other, out_mine, out_other, at_mine, at_other):
    height = rows.shape[0]
    wide = rows.astype(jnp.float32)
    inv_rms = lax.rsqrt(jnp.mean(wide * wide, axis=1, keepdims=True) + 1e-06)
    scaled = (wide * gain[...]).astype(jnp.bfloat16)
    for weight, out, at in ((mine, out_mine, at_mine), (other, out_other, at_other)):
        product = jnp.dot(scaled, weight[...], preferred_element_type=jnp.float32)
        out[at : at + height, :] = (product * inv_rms).astype(jnp.bfloat16)


def early_body(count, *refs):
    rows = refs[:count]
    gain, mine, other, cache, out_mine, out_other, held, sems, out_sems = refs[count:]
    copies = [pltpu.make_async_copy(r, held.at[k], sems.at[k]) for k, r in enumerate(rows)]
    for copy in copies:
        copy.start()
    where = places(EARLY, 0)
    stores = []
    for k, copy in enumerate(copies):
        copy.wait()
        project_block(held[k], gain, mine, other, out_mine, out_other, k * POS, k * POS)
        stores.append(store_block(out_mine, k, where[k], cache, out_sems.at[k]))
    for store in stores:
        store.wait()


def project_early(rows, gain, weights):
    count = len(rows)
    height = POS * count
    shape = pltpu.VMEM((height, WIDE), jnp.bfloat16)
    return pl.pallas_call(
        functools.partial(early_body, count),
        out_shape=(jax.ShapeDtypeStruct((2 * RING * POS, WIDE), jnp.bfloat16), shape, shape),
        in_specs=[ANY] * count + [VMEM] * 3,
        out_specs=(ANY, VMEM, VMEM),
        scratch_shapes=[
            pltpu.VMEM((count, POS, 2048), jnp.bfloat16),
            pltpu.SemaphoreType.DMA((count,)),
            pltpu.SemaphoreType.DMA((count,)),
        ],
        compiler_params=LIMIT,
        cost_estimate=pl.CostEstimate(
            flops=height * 2048 * 512, bytes_accessed=height * 2048 * 2, transcendentals=0
        ),
    )(*rows, gain, *weights)


def late_body(rows, gain, mine, other, out_mine, out_other):
    project_block(rows[...], gain, mine, other, out_mine, out_other, 0, 0)


def project_late(rows, gain, weights):
    shape = pltpu.VMEM((POS, WIDE), jnp.bfloat16)
    return pl.pallas_call(
        late_body,
        out_shape=(shape, shape),
        in_specs=[VMEM] * 4,
        out_specs=(VMEM, VMEM),
        compiler_params=LIMIT,
    )(rows, gain, *weights)


def places(kinds, partner):
    at, core = lax.axis_index("y"), lax.axis_index("c")
    sign = (1 - 2 * core) * (2 * partner - 1)
    return [
        (at + sign * hops + RING) % RING * 2 + (core + partner + crossed) % 2
        for hops, crossed in kinds
    ]


def store_block(ref, row, place, cache, sem):
    block = ref.at[row * POS : (row + 1) * POS, :]
    start = pl.multiple_of(place * POS, POS)
    copy = pltpu.make_async_copy(block, cache.at[pl.ds(start, POS), :], sem)
    copy.start()
    return copy


def read_parts(small):
    lane = lax.broadcasted_iota(jnp.int32, (2, WIDE), 1)
    head = lax.broadcasted_iota(jnp.int32, (2, WIDE), 0)
    both = jnp.broadcast_to(small[0:1, :], (2, WIDE))
    new = jnp.broadcast_to(small[1:2, :], (2, WIDE))
    fresh = jnp.sum(jnp.where(lane == head, small[2:3, :], 0.0), axis=1, keepdims=True)
    keyed = jnp.where(lane < HEAD, jnp.where(head == 0, both, pltpu.roll(both, HEAD, 1)), 0.0)
    own = jnp.sum(keyed * new, axis=1, keepdims=True) * FACTOR
    return keyed.astype(jnp.bfloat16), new, own, fresh


def finish_body(gates, small, *refs):
    cache, gate_out, read, sems = refs[-4:]
    kinds = ((EARLY, 0), (LATE, 0), (EARLY, 1), (LATE, 1))
    pieces = [(ref, places(*kind)) for ref, kind in zip(refs, kinds)]
    copies = []
    for ref, where in pieces[1:]:
        for row, place in enumerate(where):
            copies.append(store_block(ref, row, place, cache, sems.at[len(copies)]))
    gate_out[...] = jnp.concatenate([gates[p] for p in range(2 * RING)], axis=1)
    query, new, own, fresh = read_parts(small)
    top, scores = own, []
    for ref, where in pieces:
        raw = lax.dot_general(
            query, ref[...], (((1,), (1,)), ((), ())), preferred_element_type=jnp.float32
        )
        gate = jnp.concatenate([gates[place] for place in where], axis=1)
        scores.append(raw * FACTOR + fresh - gate)
        top = jnp.maximum(top, jnp.max(scores[-1], axis=1, keepdims=True))
    total = jnp.exp(own - top)
    numer = total * new
    for (ref, _), score in zip(pieces, scores):
        expo = jnp.exp(score - top)
        total += jnp.sum(expo, axis=1, keepdims=True)
        numer += jnp.dot(
            expo.astype(jnp.bfloat16), ref[...], preferred_element_type=jnp.float32
        )
    result = numer / total
    lane = lax.broadcasted_iota(jnp.int32, (1, WIDE), 1)
    shifted = pltpu.roll(result, HEAD, 1)
    read[...] = jnp.where(lane < HEAD, shifted[:1], result[1:]).astype(jnp.bfloat16)
    for copy in copies:
        copy.wait()


def finish(gates, small, pieces, cache):
    return pl.pallas_call(
        finish_body,
        out_shape=(
            jax.ShapeDtypeStruct((2 * RING * POS, WIDE), jnp.bfloat16),
            jax.ShapeDtypeStruct((2, 2 * RING * POS), jnp.float32),
            jax.ShapeDtypeStruct((1, WIDE), jnp.bfloat16),
        ),
        in_specs=[VMEM] * 6 + [ANY],
        out_specs=(ANY, VMEM, VMEM),
        scratch_shapes=[pltpu.SemaphoreType.DMA((len(EARLY) + 2 * len(LATE),))],
        input_output_aliases={6: 0},
        compiler_params=LIMIT,
    )(on_chip(gates), on_chip(small), *[on_chip(p) for p in pieces], cache)


def per_device(tokens, norm_gain, key_weight, value_weight, cum_gate, new_gate, new_query, new_kv):
    block = tokens[0]
    tp = ("y", "c")
    ahead = [lax.ppermute(block, tp, AHEAD)]

    local = jnp.concatenate([key_weight, value_weight], axis=1)
    spread = jnp.broadcast_to(local[None], (32,) + local.shape)
    gain = jnp.broadcast_to(norm_gain[None], (1, 2048))
    small = jnp.concatenate(
        [
            new_query.astype(jnp.float32),
            new_kv[0].astype(jnp.float32),
            jnp.pad(new_gate, ((0, 0), (0, WIDE - 2))),
        ],
        axis=0,
    )
    gate_parts = cum_gate[0].reshape(2 * RING, 2, POS)
    fellow = lax.ppermute(block, "c", SWAP)
    fellow, gain, small, gate_parts, spread = lax.optimization_barrier(
        (fellow, gain, small, gate_parts, spread)
    )
    crossed = [lax.ppermute(fellow, tp, AHEAD)]
    gathered = lax.all_to_all(spread, ("z", "x"), 0, 0, tiled=True)
    mine = gathered.reshape(2048, WIDE)
    weights = [on_chip(mine), on_chip(lax.ppermute(mine, "c", SWAP))]

    for step in (2, 3, 4):
        ahead.append(lax.ppermute(ahead[-1], tp, AHEAD))
        if step < 4:
            crossed.append(lax.ppermute(crossed[-1], tp, AHEAD))
    gates = lax.all_to_all(gate_parts, tp, split_axis=0, concat_axis=0, tiled=True)

    gain = on_chip(gain)
    first = [block]
    for pair in zip(ahead, crossed):
        first += pair
    cache, early, other = project_early(first, gain, weights)
    early_swapped = lax.ppermute(other, "c", SWAP)
    late, late_other = project_late(on_chip(ahead[3]), gain, weights)
    late_swapped = lax.ppermute(late_other, "c", SWAP)
    pieces = (early, late, early_swapped, late_swapped)
    cache, gate_out, read = finish(gates, small, pieces, cache)
    return (cache[None, None], gate_out[None], read)


def solution(mesh):
    fine = Mesh(mesh.devices.reshape(8, 4, 8, 2), ("z", "x", "y", "c"))
    sp, tp = ("z", "x"), ("y", "c")
    in_specs = (
        P(sp, tp, None),
        P(),
        P(sp, tp),
        P(sp, tp),
        P(sp, None, tp),
        P(sp, tp),
        P(sp, tp),
        P(sp, tp, None),
    )
    out_specs = (P(sp, tp, None, None), P(sp, tp, None), P(sp, tp))
    return jax.shard_map(
        per_device, mesh=fine, in_specs=in_specs, out_specs=out_specs, check_vma=False
    )
```

```python
import functools
import math

import jax
import jax.numpy as jnp
from jax import lax
from jax.experimental import pallas as pl
from jax.experimental.pallas import tpu as pltpu
from jax.sharding import Mesh, PartitionSpec as P

HEAD = 64
WIDE = 2 * HEAD
RING = 8
POS = 192
AHEAD = [(2 * y + c, 2 * ((y + 1 - 2 * c) % RING) + c) for y in range(RING) for c in (0, 1)]
SWAP = [(0, 1), (1, 0)]
FACTOR = 1.0 / math.sqrt(HEAD)
EARLY = ((0, 0), (1, 0), (1, 1), (2, 0), (2, 1), (3, 0), (3, 1))
LATE = ((4, 0),)
VMEM = pl.BlockSpec(memory_space=pltpu.VMEM)
ANY = pl.BlockSpec(memory_space=pl.ANY)
LIMIT = pltpu.CompilerParams(vmem_limit_bytes=16 * 2**20)


def on_chip(array):
    return pltpu.with_memory_space_constraint(array, pltpu.VMEM)


def project_block(rows, gain, mine, other, out_mine, out_other, at_mine, at_other):
    height = rows.shape[0]
    wide = rows.astype(jnp.float32)
    inv_rms = lax.rsqrt(jnp.mean(wide * wide, axis=1, keepdims=True) + 1e-06)
    scaled = (wide * gain[...]).astype(jnp.bfloat16)
    for weight, out, at in ((mine, out_mine, at_mine), (other, out_other, at_other)):
        product = jnp.dot(scaled, weight[...], preferred_element_type=jnp.float32)
        out[at : at + height, :] = (product * inv_rms).astype(jnp.bfloat16)


def raw_scores(query, ref):
    return lax.dot_general(
        query, ref[...], (((1,), (1,)), ((), ())), preferred_element_type=jnp.float32
    )


def early_body(count, *refs):
    rows = refs[:count]
    gain, mine, other, small, cache, out_mine, out_other, raw, held, sems, out_sems = refs[count:]
    copies = [pltpu.make_async_copy(r, held.at[k], sems.at[k]) for k, r in enumerate(rows)]
    for copy in copies:
        copy.start()
    where = places(EARLY, 0)
    stores = []
    for k, copy in enumerate(copies):
        copy.wait()
        project_block(held[k], gain, mine, other, out_mine, out_other, k * POS, k * POS)
        stores.append(store_block(out_mine, k, where[k], cache, out_sems.at[k]))
    raw[...] = raw_scores(read_parts(small)[0], out_mine)
    for store in stores:
        store.wait()


def project_early(rows, gain, weights, small):
    count = len(rows)
    height = POS * count
    shape = pltpu.VMEM((height, WIDE), jnp.bfloat16)
    return pl.pallas_call(
        functools.partial(early_body, count),
        out_shape=(
            jax.ShapeDtypeStruct((2 * RING * POS, WIDE), jnp.bfloat16),
            shape,
            shape,
            pltpu.VMEM((2, height), jnp.float32),
        ),
        in_specs=[ANY] * count + [VMEM] * 4,
        out_specs=(ANY, VMEM, VMEM, VMEM),
        scratch_shapes=[
            pltpu.VMEM((count, POS, 2048), jnp.bfloat16),
            pltpu.SemaphoreType.DMA((count,)),
            pltpu.SemaphoreType.DMA((count,)),
        ],
        compiler_params=LIMIT,
        cost_estimate=pl.CostEstimate(
            flops=height * 2048 * 512, bytes_accessed=height * 2048 * 2, transcendentals=0
        ),
    )(*rows, gain, *weights, small)


def late_body(rows, gain, mine, other, out_mine, out_other):
    project_block(rows[...], gain, mine, other, out_mine, out_other, 0, 0)


def project_late(rows, gain, weights):
    shape = pltpu.VMEM((POS, WIDE), jnp.bfloat16)
    return pl.pallas_call(
        late_body,
        out_shape=(shape, shape),
        in_specs=[VMEM] * 4,
        out_specs=(VMEM, VMEM),
        compiler_params=LIMIT,
    )(rows, gain, *weights)


def places(kinds, partner):
    at, core = lax.axis_index("y"), lax.axis_index("c")
    sign = (1 - 2 * core) * (2 * partner - 1)
    return [
        (at + sign * hops + RING) % RING * 2 + (core + partner + crossed) % 2
        for hops, crossed in kinds
    ]


def store_block(ref, row, place, cache, sem):
    block = ref.at[row * POS : (row + 1) * POS, :]
    start = pl.multiple_of(place * POS, POS)
    copy = pltpu.make_async_copy(block, cache.at[pl.ds(start, POS), :], sem)
    copy.start()
    return copy


def read_parts(small):
    lane = lax.broadcasted_iota(jnp.int32, (2, WIDE), 1)
    head = lax.broadcasted_iota(jnp.int32, (2, WIDE), 0)
    both = jnp.broadcast_to(small[0:1, :], (2, WIDE))
    new = jnp.broadcast_to(small[1:2, :], (2, WIDE))
    fresh = jnp.sum(jnp.where(lane == head, small[2:3, :], 0.0), axis=1, keepdims=True)
    keyed = jnp.where(lane < HEAD, jnp.where(head == 0, both, pltpu.roll(both, HEAD, 1)), 0.0)
    own = jnp.sum(keyed * new, axis=1, keepdims=True) * FACTOR
    return keyed.astype(jnp.bfloat16), new, own, fresh


def finish_body(gates, small, first_raw, *refs):
    cache, gate_out, read, sems = refs[-4:]
    kinds = ((EARLY, 0), (LATE, 0), (EARLY, 1), (LATE, 1))
    pieces = [(ref, places(*kind)) for ref, kind in zip(refs, kinds)]
    copies = []
    for ref, where in pieces[1:]:
        for row, place in enumerate(where):
            copies.append(store_block(ref, row, place, cache, sems.at[len(copies)]))
    gate_out[...] = jnp.concatenate([gates[p] for p in range(2 * RING)], axis=1)
    query, new, own, fresh = read_parts(small)
    top, scores = own, []
    for ref, where in pieces:
        raw = raw_scores(query, ref) if scores else first_raw[...]
        gate = jnp.concatenate([gates[place] for place in where], axis=1)
        scores.append(raw * FACTOR + fresh - gate)
        top = jnp.maximum(top, jnp.max(scores[-1], axis=1, keepdims=True))
    total = jnp.exp(own - top)
    numer = total * new
    for (ref, _), score in zip(pieces, scores):
        expo = jnp.exp(score - top)
        total += jnp.sum(expo, axis=1, keepdims=True)
        numer += jnp.dot(
            expo.astype(jnp.bfloat16), ref[...], preferred_element_type=jnp.float32
        )
    result = numer / total
    lane = lax.broadcasted_iota(jnp.int32, (1, WIDE), 1)
    shifted = pltpu.roll(result, HEAD, 1)
    read[...] = jnp.where(lane < HEAD, shifted[:1], result[1:]).astype(jnp.bfloat16)
    for copy in copies:
        copy.wait()


def finish(gates, small, raw, pieces, cache):
    return pl.pallas_call(
        finish_body,
        out_shape=(
            jax.ShapeDtypeStruct((2 * RING * POS, WIDE), jnp.bfloat16),
            jax.ShapeDtypeStruct((2, 2 * RING * POS), jnp.float32),
            jax.ShapeDtypeStruct((1, WIDE), jnp.bfloat16),
        ),
        in_specs=[VMEM] * 7 + [ANY],
        out_specs=(ANY, VMEM, VMEM),
        scratch_shapes=[pltpu.SemaphoreType.DMA((len(EARLY) + 2 * len(LATE),))],
        input_output_aliases={7: 0},
        compiler_params=LIMIT,
    )(on_chip(gates), on_chip(small), on_chip(raw), *[on_chip(p) for p in pieces], cache)


def per_device(tokens, norm_gain, key_weight, value_weight, cum_gate, new_gate, new_query, new_kv):
    block = tokens[0]
    tp = ("y", "c")
    ahead = [lax.ppermute(block, tp, AHEAD)]

    local = jnp.concatenate([key_weight, value_weight], axis=1)
    spread = jnp.broadcast_to(local[None], (32,) + local.shape)
    gain = jnp.broadcast_to(norm_gain[None], (1, 2048))
    small = jnp.concatenate(
        [
            new_query.astype(jnp.float32),
            new_kv[0].astype(jnp.float32),
            jnp.pad(new_gate, ((0, 0), (0, WIDE - 2))),
        ],
        axis=0,
    )
    gate_parts = cum_gate[0].reshape(2 * RING, 2, POS)
    fellow = lax.ppermute(block, "c", SWAP)
    fellow, gain, small, gate_parts, spread = lax.optimization_barrier(
        (fellow, gain, small, gate_parts, spread)
    )
    crossed = [lax.ppermute(fellow, tp, AHEAD)]
    gathered = lax.all_to_all(spread, ("z", "x"), 0, 0, tiled=True)
    mine = gathered.reshape(2048, WIDE)
    weights = [on_chip(mine), on_chip(lax.ppermute(mine, "c", SWAP))]

    for step in (2, 3, 4):
        ahead.append(lax.ppermute(ahead[-1], tp, AHEAD))
        if step < 4:
            crossed.append(lax.ppermute(crossed[-1], tp, AHEAD))
    gates = lax.all_to_all(gate_parts, tp, split_axis=0, concat_axis=0, tiled=True)

    gain = on_chip(gain)
    first = [block]
    for pair in zip(ahead, crossed):
        first += pair
    cache, early, other, raw = project_early(first, gain, weights, on_chip(small))
    early_swapped = lax.ppermute(other, "c", SWAP)
    late, late_other = project_late(on_chip(ahead[3]), gain, weights)
    late_swapped = lax.ppermute(late_other, "c", SWAP)
    pieces = (early, late, early_swapped, late_swapped)
    cache, gate_out, read = finish(gates, small, raw, pieces, cache)
    return (cache[None, None], gate_out[None], read)


def solution(mesh):
    fine = Mesh(mesh.devices.reshape(8, 4, 8, 2), ("z", "x", "y", "c"))
    sp, tp = ("z", "x"), ("y", "c")
    in_specs = (
        P(sp, tp, None),
        P(),
        P(sp, tp),
        P(sp, tp),
        P(sp, None, tp),
        P(sp, tp),
        P(sp, tp),
        P(sp, tp, None),
    )
    out_specs = (P(sp, tp, None, None), P(sp, tp, None), P(sp, tp))
    return jax.shard_map(
        per_device, mesh=fine, in_specs=in_specs, out_specs=out_specs, check_vma=False
    )
```
